256 devices in a mesh: grp: 2 (over y), kv: 16 (over z), tp: 8 (over x, core).
Axes of the slice: x: 4, y: 2, z: 16, core: 2. Of those that a mesh axis runs over, the one named last changes fastest.
The devices are a block of a 4x16x16 slice.
Arguments:
- stream: bfloat16 [256, 2048], P('grp', ('kv', 'tp')), parts along dimension 0, may hold values from -72 to 72
- lengths: int32 [256], P(('grp', 'kv')), parts along dimension 0, may hold values from 1 to 8, 384 in all
- delta_state: float32 [256, 32, 128, 128], P(('grp', 'kv'), 'tp'), parts along dimension 0, may hold values from -0.6 to 0.6
- q_hist: bfloat16 [256, 3, 2048], P(('grp', 'kv'), None, 'tp'), parts along dimension 0, may hold values from -6 to 6
- k_hist: bfloat16 [256, 3, 2048], P(('grp', 'kv'), None, 'tp'), parts along dimension 0, may hold values from -6 to 6
- v_hist: bfloat16 [256, 3, 4096], P(('grp', 'kv'), None, 'tp'), parts along dimension 0, may hold values from -6 to 6
- norm_gain: bfloat16 [2048], replicated, may hold values from 0.099609375 to 1.8984375
- w_query: bfloat16 [2048, 2048], P('kv', 'tp'), may hold values from -0.125 to 0.125
- w_key: bfloat16 [2048, 2048], P('kv', 'tp'), may hold values from -0.125 to 0.125
- w_value: bfloat16 [2048, 4096], P('kv', 'tp'), may hold values from -0.125 to 0.125
- w_gate: bfloat16 [2048, 4096], P('kv', 'tp'), may hold values from -0.125 to 0.125
- w_beta: bfloat16 [2048, 32], replicated, may hold values from -0.125 to 0.125
- w_decay: bfloat16 [2048, 32], replicated, may hold values from -0.125 to 0.125
- conv_query: bfloat16 [4, 2048], replicated, may hold values from -3 to 3
- conv_key: bfloat16 [4, 2048], replicated, may hold values from -3 to 3
- conv_value: bfloat16 [4, 4096], replicated, may hold values from -3 to 3
- decay_log: float32 [32], replicated, may hold values from 0 to 2.77
- time_bias: float32 [32], replicated, may hold values from -4 to 0
- out_gain: bfloat16 [128], replicated, may hold values from 0.099609375 to 1.8984375
- w_out: bfloat16 [4096, 2048], P('tp', 'kv'), may hold values from -0.09375 to 0.09375
- mlp_gain: bfloat16 [2048], replicated, may hold values from 0.099609375 to 1.8984375
- w_up: bfloat16 [2048, 8192], P('kv', 'tp'), may hold values from -0.125 to 0.125
- w_down: bfloat16 [8192, 2048], P('tp', 'kv'), may hold values from -0.0625 to 0.0625
Outputs:
- result: bfloat16 [256, 2048], P('grp', ('kv', 'tp')), parts along dimension 0
- new_state: float32 [256, 32, 128, 128], P(('grp', 'kv'), 'tp'), parts along dimension 0
The draws below stay inside these ranges and needn't reach their ends.
There are 2 independent parts, one for each index of `grp`. The reference program is written for one: setup_inputs(seed, part) draws one part's arguments, and reference() takes and returns one part's arrays. A program takes and returns all parts, laid end to end along the dimension named above; an argument that names none is the same for every part. Nothing has to cross between parts.
All inputs are finite; a program needn't handle non-finite values. No bound on the sum of `lengths` on one device may be relied on, other than what follows from the above.
Results may differ from the reference program's by a relative error of at most 0.01.
Values may be sent and summed in bfloat16 or wider, within the bound.
A program may use at most 64 MiB of HBM per device.

```python
import math
import jax
import jax.numpy as jnp
import numpy as np
from jax import lax

D = 2048
HEADS_K = 16
HEADS_V = 32
HEAD_DIM = 128
FF_UNITS = 8192
CONV = 4
SEQS = 128
N_KV = 16
N_TP = 8


def draw_stream(key, part):
    first_key, second_key, third_key = jax.random.split(jax.random.fold_in(key, 11), 3)
    columns = jnp.arange(D)
    block_number = columns // (D // N_KV)
    piece_number = columns // (D // (N_KV * N_TP)) % N_TP
    rising = 3.0 ** (block_number / max(N_KV - 1, 1)) * 3.0 ** (piece_number / max(N_TP - 1, 1))
    roughness = jax.random.uniform(first_key, (D,), jnp.float32, 0.5, 1.5)
    row_factor = jnp.exp(jax.random.uniform(second_key, (SEQS, 1), jnp.float32, 0.0, math.log(4.0)))
    base_values = jnp.clip(jax.random.normal(third_key, (SEQS, D), jnp.float32), -4.0, 4.0)
    return (base_values * rising * roughness * row_factor / 3.0).astype(jnp.bfloat16)


def block_scale(own_key, extent, cuts, smallest, largest):
    def one(dim, parts):
        steps = jax.random.uniform(jax.random.fold_in(jax.random.fold_in(own_key, 6), dim), (parts,), jnp.float32, smallest / len(cuts), largest / len(cuts))
        return jnp.repeat(jnp.exp(steps), extent[dim] // parts).reshape((-1,) + (1,) * (len(extent) - dim - 1))

    loudness = one(*cuts[0])
    for cut in cuts[1:]:
        loudness = loudness * one(*cut)
    return loudness


def profile(amount, total, reach, skew):
    portions = [(1 << 20) // math.isqrt(standing ** skew) + 1 for standing in range(2, amount + 1)]
    surplus, holding = total - reach - (amount - 1), [1] * (amount - 1)
    while surplus > 0:
        movable = [i for i in range(amount - 1) if holding[i] < reach]
        whole, remaining = sum([portions[i] for i in movable]), surplus
        for i in movable:
            extra = min(reach - holding[i], max(1, remaining * portions[i] // whole), surplus)
            holding[i] = holding[i] + extra
            surplus = surplus - extra
    return np.array([reach] + holding)


def uneven(rng, count, total, most, skew):
    if count == 2:
        one = jax.random.randint(rng, (), max(1, total - most), min(most, total - 1) + 1)
        return jnp.stack([one, total - one])
    sizes = jnp.asarray(profile(count, total, most, skew), jnp.int32)
    pairs = (count - 1) // 2
    donor, taker = sizes[1:1 + 2 * pairs:2], sizes[2:2 + 2 * pairs:2]
    room = jnp.minimum(donor - 1, most - taker)
    passed = jax.random.randint(jax.random.fold_in(rng, 1), (pairs,), 0, 1 << 20) % (room + 1)
    sizes = sizes.at[1:1 + 2 * pairs:2].set(donor - passed).at[2:2 + 2 * pairs:2].set(taker + passed)
    return sizes[jax.random.permutation(jax.random.fold_in(rng, 2), count)]


def normal_values(rng, extent, scale, most, cuts=(), held_as=jnp.bfloat16):
    drawn = scale * jax.random.normal(rng, extent, jnp.float32)
    if cuts:
        drawn = drawn * block_scale(rng, extent, cuts, -0.22, 0.18)
    return jnp.clip(drawn, -most, most).astype(held_as)


def setup_inputs(seed: int = 0, part: int = 0) -> dict:
    key_list = jax.random.split(jax.random.key(seed), 24)
    own_keys = jax.random.split(jax.random.fold_in(key_list[23], part), 24)
    stream = draw_stream(jax.random.fold_in(jax.random.fold_in(key_list[23], part), 71), part)
    lengths = uneven(own_keys[1], SEQS, 3 * SEQS, 8, 2).astype(jnp.int32)
    delta_state = normal_values(own_keys[2], (SEQS, HEADS_V, HEAD_DIM, HEAD_DIM), 0.1, 0.6, ((0, 16), (1, 8)), jnp.float32)
    q_hist = normal_values(own_keys[3], (SEQS, CONV - 1, HEADS_K * HEAD_DIM), 1.0, 6.0, ((0, 16), (2, 8)))
    k_hist = normal_values(own_keys[4], (SEQS, CONV - 1, HEADS_K * HEAD_DIM), 1.0, 6.0, ((0, 16), (2, 8)))
    v_hist = normal_values(own_keys[5], (SEQS, CONV - 1, HEADS_V * HEAD_DIM), 1.0, 6.0, ((0, 16), (2, 8)))
    norm_gain = jnp.clip(1.0 + 0.18 * jax.random.normal(key_list[6], (D,), jnp.float32), 0.099609375, 1.8984375).astype(jnp.bfloat16)
    w_query = normal_values(key_list[7], (D, HEADS_K * HEAD_DIM), D ** -0.5, 0.125, ((0, 16), (1, 8)))
    w_key = normal_values(key_list[8], (D, HEADS_K * HEAD_DIM), D ** -0.5, 0.125, ((0, 16), (1, 8)))
    w_value = normal_values(key_list[9], (D, HEADS_V * HEAD_DIM), D ** -0.5, 0.125, ((0, 16), (1, 8)))
    w_gate = normal_values(key_list[10], (D, HEADS_V * HEAD_DIM), D ** -0.5, 0.125, ((0, 16), (1, 8)))
    w_beta = normal_values(key_list[11], (D, HEADS_V), D ** -0.5, 0.125)
    w_decay = normal_values(key_list[12], (D, HEADS_V), D ** -0.5, 0.125)
    conv_query = normal_values(key_list[13], (CONV, HEADS_K * HEAD_DIM), CONV ** -0.5, 3.0)
    conv_key = normal_values(key_list[14], (CONV, HEADS_K * HEAD_DIM), CONV ** -0.5, 3.0)
    conv_value = normal_values(key_list[15], (CONV, HEADS_V * HEAD_DIM), CONV ** -0.5, 3.0)
    decay_log = jnp.clip(jax.random.uniform(key_list[16], (HEADS_V,), jnp.float32, 0.0, 2.77), 0.0, 2.77)
    time_bias = jnp.clip(jax.random.uniform(key_list[17], (HEADS_V,), jnp.float32, -4.0, 0.0), -4.0, 0.0)
    out_gain = jnp.clip(1.0 + 0.18 * jax.random.normal(key_list[18], (HEAD_DIM,), jnp.float32), 0.099609375, 1.8984375).astype(jnp.bfloat16)
    w_out = normal_values(key_list[19], (HEADS_V * HEAD_DIM, D), (HEADS_V * HEAD_DIM) ** -0.5, 0.09375, ((0, 8), (1, 16)))
    mlp_gain = jnp.clip(1.0 + 0.18 * jax.random.normal(key_list[20], (D,), jnp.float32), 0.099609375, 1.8984375).astype(jnp.bfloat16)
    w_up = normal_values(key_list[21], (D, FF_UNITS), D ** -0.5, 0.125, ((0, 16), (1, 8)))
    w_down = normal_values(key_list[22], (FF_UNITS, D), FF_UNITS ** -0.5, 0.0625, ((0, 8), (1, 16)))
    return {"stream": stream, "lengths": lengths, "delta_state": delta_state, "q_hist": q_hist, "k_hist": k_hist, "v_hist": v_hist, "norm_gain": norm_gain, "w_query": w_query, "w_key": w_key, "w_value": w_value, "w_gate": w_gate, "w_beta": w_beta, "w_decay": w_decay, "conv_query": conv_query, "conv_key": conv_key, "conv_value": conv_value, "decay_log": decay_log, "time_bias": time_bias, "out_gain": out_gain, "w_out": w_out, "mlp_gain": mlp_gain, "w_up": w_up, "w_down": w_down}


EPSILON = 1e-06

def unit_rows(values, factor):
    return values * lax.rsqrt(lax.optimization_barrier(jnp.sum(values * values, axis=-1, keepdims=True)) + EPSILON) * factor

def short_filter(current, history, weights, live_rows):
    history_live = jnp.where(live_rows[:, :, None], history.astype(jnp.float32), 0.0)
    filter_taps = weights.astype(jnp.float32)
    filtered = current * filter_taps[-1] + lax.optimization_barrier(jnp.sum(history_live * filter_taps[None, :-1], axis=1))
    return jax.nn.silu(filtered)

def delta_step(delta_state, fresh_rows, queries, keys_now, values_now, strength, log_fade):
    fade_factor = jnp.exp(log_fade)[:, :, None, None]
    carried = jnp.where(fresh_rows[:, None, None, None], 0.0, delta_state) * fade_factor
    recalled = lax.optimization_barrier(jnp.sum(carried * keys_now[:, :, :, None], axis=2))
    update = strength[:, :, None] * (values_now - recalled)
    new_state = carried + keys_now[:, :, :, None] * update[:, :, None, :]
    readout = lax.optimization_barrier(jnp.sum(new_state * queries[:, :, :, None], axis=2))
    return (new_state, readout)

def gated_norm(readout, gain, gate_in):
    normed = readout * lax.rsqrt(lax.optimization_barrier(jnp.mean(readout * readout, axis=-1, keepdims=True)) + EPSILON)
    return (normed * gain.astype(jnp.float32) * jax.nn.silu(gate_in)).astype(jnp.bfloat16)

def reference(stream, lengths, delta_state, q_hist, k_hist, v_hist, norm_gain, w_query, w_key, w_value, w_gate, w_beta, w_decay, conv_query, conv_key, conv_value, decay_log, time_bias, out_gain, w_out, mlp_gain, w_up, w_down):
    sequences = stream.shape[0]
    stream_wide = stream.astype(jnp.float32)
    row_scale = lax.rsqrt(lax.optimization_barrier(jnp.sum(stream_wide * stream_wide, axis=1, keepdims=True)) / D + EPSILON)
    scaled = (stream_wide * norm_gain.astype(jnp.float32)).astype(jnp.bfloat16)

    def project(weight):
        return jnp.dot(scaled, weight, preferred_element_type=jnp.float32) * row_scale
    live_rows = jnp.arange(CONV - 1, dtype=jnp.int32)[None, :] >= (CONV - lengths)[:, None]
    queries = short_filter(project(w_query), q_hist, conv_query, live_rows)
    keys_now = short_filter(project(w_key), k_hist, conv_key, live_rows)
    values_now = short_filter(project(w_value), v_hist, conv_value, live_rows)
    gate_in = project(w_gate).reshape(sequences, HEADS_V, HEAD_DIM)
    repeat_count = HEADS_V // HEADS_K
    queries = jnp.repeat(unit_rows(queries.reshape(sequences, HEADS_K, HEAD_DIM), HEAD_DIM ** (-0.5)), repeat_count, axis=1)
    keys_now = jnp.repeat(unit_rows(keys_now.reshape(sequences, HEADS_K, HEAD_DIM), 1.0), repeat_count, axis=1)
    values_now = values_now.reshape(sequences, HEADS_V, HEAD_DIM)
    strength = jax.nn.sigmoid(project(w_beta))
    log_fade = -jnp.exp(decay_log) * jax.nn.softplus(project(w_decay) + time_bias)
    new_state, readout = delta_step(delta_state, lengths == 1, queries, keys_now, values_now, strength, log_fade)
    gated = gated_norm(readout, out_gain, gate_in).reshape(sequences, HEADS_V * HEAD_DIM)
    mixed = (stream_wide + jnp.dot(gated, w_out, preferred_element_type=jnp.float32)).astype(jnp.bfloat16)
    mixed_wide = mixed.astype(jnp.float32)
    unit_scale = lax.rsqrt(lax.optimization_barrier(jnp.sum(mixed_wide * mixed_wide, axis=1, keepdims=True)) / D + EPSILON)
    scaled_mix = (mixed_wide * mlp_gain.astype(jnp.float32)).astype(jnp.bfloat16)
    unit_terms = jnp.dot(scaled_mix, w_up, preferred_element_type=jnp.float32) * unit_scale
    hidden = jnp.square(jax.nn.relu(unit_terms)).astype(jnp.bfloat16)
    result = (mixed_wide + jnp.dot(hidden, w_down, preferred_element_type=jnp.float32)).astype(jnp.bfloat16)
    return (result, new_state)
```

```python
import functools
import types
import typing

import jax
import jax.numpy as jnp
from jax import lax
from jax.experimental import pallas as pl
from jax.experimental.pallas import tpu as pltpu
from jax.sharding import PartitionSpec as P

EPSILON = 1e-06
LANES = 128
MESH = pl.DeviceIdType.MESH
F32 = jnp.float32
BF16 = jnp.bfloat16

class Inputs(typing.NamedTuple):
    stream: typing.Any
    lengths: typing.Any
    delta_state: typing.Any
    q_hist: typing.Any
    k_hist: typing.Any
    v_hist: typing.Any
    norm_gain: typing.Any
    w_query: typing.Any
    w_key: typing.Any
    w_value: typing.Any
    w_gate: typing.Any
    w_beta: typing.Any
    w_decay: typing.Any
    conv_query: typing.Any
    conv_key: typing.Any
    conv_value: typing.Any
    decay_log: typing.Any
    time_bias: typing.Any
    out_gain: typing.Any
    w_out: typing.Any
    mlp_gain: typing.Any
    w_up: typing.Any
    w_down: typing.Any


def ring_offsets(n):
    return list(range(1, n // 2 + 1)) + [-o for o in range(1, (n + 1) // 2)]


def tree(n, relayed):
    return {o: (o - (1 if o > 0 else -1)) if abs(o) in relayed else 0 for o in ring_offsets(n)}


def children_of(parents, o):
    return [c for c, p in parents.items() if p == o]


def depth_of(parents, o):
    return 0 if o == 0 else 1 + depth_of(parents, parents[o])


class Exchange:
    def __init__(self, axis, n, place, send_sems, recv_sems):
        self.axis, self.n, self.place = axis, n, place
        self.send_sems, self.recv_sems = send_sems, recv_sems
        self.started = []

    def at(self, o):
        return lax.rem(self.place + (o + self.n), self.n)

    def copy(self, key, hop, src, dst):
        slot = key % self.n
        return pltpu.make_async_remote_copy(
            src_ref=src,
            dst_ref=dst,
            send_sem=self.send_sems.at[slot],
            recv_sem=self.recv_sems.at[slot],
            device_id={self.axis: self.at(hop)},
            device_id_type=MESH,
        )

    def start(self, key, hop, src, dst):
        copy = self.copy(key, hop, src, dst)
        copy.start()
        self.started.append(copy)

    def wait(self, key, src, dst):
        self.copy(key, 1, src, dst).wait_recv()

    def drain(self):
        for copy in self.started:
            copy.wait_send()
        self.started = []


class Scatter:
    def __init__(self, exchange, parents, part, send, recv):
        self.x, self.parents = exchange, parents
        self.part, self.send, self.recv = part, send, recv
        self.inner = [o for o in parents if children_of(parents, o)]
        self.inner.sort(key=lambda o: (-depth_of(parents, o), -abs(o)))

    def _send(self, o, value):
        slot = o % self.x.n
        self.send[slot] = value.astype(BF16)
        self.x.start(o, o - self.parents[o], self.send.at[slot], self.recv.at[slot])

    def _gather(self, o):
        total = self.part[o % self.x.n]
        for c in children_of(self.parents, o):
            slot = c % self.x.n
            self.x.wait(c, self.send.at[slot], self.recv.at[slot])
            total = total + self.recv[slot].astype(F32)
        return total

    def leaves(self, relayed):
        for o in sorted(self.parents, key=lambda o: -abs(o)):
            if o not in self.inner and (self.parents[o] != 0) == relayed:
                self._send(o, self.part[o % self.x.n])

    def hubs(self):
        for o in self.inner:
            self._send(o, self._gather(o))

    def total(self):
        return self._gather(0)


class Gather:
    def __init__(self, exchange, parents, blocks):
        self.x, self.parents, self.blocks = exchange, parents, blocks

    def _forward(self, o):
        source = self.blocks.at[self.x.at(-o)]
        for c in sorted(children_of(self.parents, o), key=lambda c: -abs(c)):
            self.x.start(c, c - o, source, source)

    def begin(self):
        self._forward(0)

    def finish(self):
        order = sorted(self.parents, key=lambda o: (not children_of(self.parents, o), abs(o)))
        for o in order:
            block = self.blocks.at[self.x.at(-o)]
            self.x.wait(o, block, block)
            self._forward(o)


def rows_of(blocks):
    return blocks.reshape(blocks.shape[0] * blocks.shape[1], blocks.shape[2])


def softplus(x):
    return jnp.maximum(x, 0.0) + jnp.log1p(jnp.exp(-jnp.abs(x)))


class Phases:
    def __init__(self):
        self.scope = None

    def __call__(self, label):
        self.end()
        self.scope = jax.named_scope(label)
        self.scope.__enter__()

    def end(self):
        if self.scope is not None:
            self.scope.__exit__(None, None, None)
        self.scope = None


def layer(d, a, result, new_state, v, r):
    n_kv, n_tp = d.n_kv, d.n_tp
    own, heads, size = d.own, d.heads, d.size
    key_cols, value_cols, ff = d.key_cols, d.value_cols, d.ff
    width, block, piece, taps = d.width, d.block, d.piece, d.taps
    heads_all, seqs = d.heads_all, d.own * d.n_kv
    kv, tp = lax.axis_index("kv"), lax.axis_index("tp")
    phase = Phases()
    phase("enter")

    def over_kv(sems):
        return Exchange("kv", n_kv, kv, *sems)

    def over_tp(sems):
        return Exchange("tp", n_tp, tp, *sems)

    x_stream = over_tp(r.stream_sems)
    x_proj = over_kv(r.proj_sems)
    barrier = pltpu.get_barrier_semaphore()
    for o in range(1, n_tp):
        pl.semaphore_signal(barrier, 1, device_id={"tp": x_stream.at(o)}, device_id_type=MESH)
    for o in (1, -1):
        pl.semaphore_signal(barrier, 1, device_id={"kv": x_proj.at(o)}, device_id_type=MESH)

    started = []

    def load(source, into):
        copy = pltpu.make_async_copy(source, into, r.load_sems.at[len(started)])
        copy.start()
        started.append(copy)
        return copy

    def tp_cols(ref, count):
        return ref.at[:, pl.ds(pl.multiple_of(tp * count, LANES), count)]

    def kv_cols(ref):
        return ref.at[:, pl.ds(pl.multiple_of(kv * block, LANES), block)]

    sources = a._replace(
        w_beta=kv_cols(a.w_beta),
        w_decay=kv_cols(a.w_decay),
        conv_query=tp_cols(a.conv_query, key_cols),
        conv_key=tp_cols(a.conv_key, key_cols),
        conv_value=tp_cols(a.conv_value, value_cols),
    )
    first = Inputs(*range(len(a)))
    order = [first.stream, first.norm_gain, first.w_decay, first.w_beta]
    order += [first.w_query, first.w_key, first.w_value, first.w_gate]
    order += [i for i in range(len(a)) if i not in order]
    order.remove(first.delta_state)
    order.append(first.delta_state)
    copies = {i: load(sources[i], v[i]) for i in order}
    c = Inputs(*[copies[i] for i in range(len(a))])

    c.stream.wait()
    pieces = r.pieces
    pieces[tp] = v.stream[...]
    pl.semaphore_wait(barrier, n_tp - 1 + 2)

    def tell(step):
        sem = r.near_sems.at[step.bit_length() - 1]
        for o in (step, -step):
            pl.semaphore_signal(sem, 1, device_id={"kv": x_proj.at(o)}, device_id_type=MESH)

    def heard(step):
        pl.semaphore_wait(r.near_sems.at[step.bit_length() - 1], 2)

    g_stream = Gather(x_stream, {o: 0 for o in ring_offsets(n_tp)}, pieces)
    g_stream.begin()
    tell(1)

    def gain_row(copy, ref):
        copy.wait()
        gains = ref[...].astype(F32)
        row = lax.broadcasted_iota(jnp.int32, gains.shape, 0)
        return jnp.sum(jnp.where(row == kv, gains, 0.0), axis=0, keepdims=True)

    norm_row = gain_row(c.norm_gain, v.norm_gain)
    c.w_decay.wait()
    c.w_beta.wait()
    idle = jnp.zeros((LANES - 2 * heads_all, block), F32)
    w_rates = [v.w_decay[...].astype(F32), v.w_beta[...].astype(F32), idle]
    w_rates = jnp.concatenate(w_rates, axis=0).astype(BF16)
    for copy in (c.w_query, c.w_key, c.w_value, c.w_gate):
        copy.wait()

    parents = d.scatter_tree
    order = [0] + list(parents)

    def by_owner(values):
        r.rows[...] = values.reshape(n_kv, own, block)
        return jnp.concatenate([r.rows[x_proj.at(o)] for o in order], axis=0)

    def put(part, at, product):
        parts = product.reshape(n_kv, own, product.shape[1])
        for i, o in enumerate(order):
            part[o % n_kv, :, at : at + product.shape[1]] = parts[i]

    def spread_squares(values):
        squares = jnp.sum(values * values, axis=1, keepdims=True)
        return by_owner(jnp.broadcast_to(squares, values.shape))

    phase("stream")
    g_stream.finish()
    phase("project")
    stream_block = rows_of(pieces[...].astype(F32)).T
    r.stream_block[...] = stream_block
    lhs = by_owner((stream_block * norm_row).astype(BF16).astype(F32)).astype(BF16)
    at = 0
    for weight in (v.w_query, v.w_key, v.w_value):
        product = jnp.dot(lhs, weight[...], preferred_element_type=F32)
        put(r.part_a, at, product)
        at += product.shape[1]
    rates = lax.dot_general(lhs, w_rates, (((1,), (1,)), ((), ())), preferred_element_type=F32)
    lane = lax.broadcasted_iota(jnp.int32, rates.shape, 1)
    put(r.part_a, at, jnp.where(lane < 2 * heads_all, rates, spread_squares(stream_block)))
    s_proj = Scatter(x_proj, parents, r.part_a, r.send_a, r.recv_a)
    s_proj.leaves(True)
    heard(1)
    tell(2)
    put(r.part_g, 0, jnp.dot(lhs, v.w_gate[...], preferred_element_type=F32))
    s_gate = Scatter(over_kv(r.gate_sems), parents, r.part_g, r.send_g, r.recv_g)
    heard(2)
    tell(4)

    phase("history")
    c.lengths.wait()
    seq = lax.broadcasted_iota(jnp.int32, (own, LANES), 0)
    lens = jnp.zeros((own, LANES), jnp.int32)
    for s in range(own):
        lens = jnp.where(seq == s, v.lengths[s], lens)

    def history(past_copy, past, weight_copy, weight):
        past_copy.wait()
        weight_copy.wait()
        weights = weight[...].astype(F32)
        count = weights.shape[1]
        wide = jnp.concatenate([lens] * (count // LANES), axis=1)
        total = jnp.zeros((own, count), F32)
        for i in range(taps - 1):
            term = past[i].astype(F32) * weights[i : i + 1, :]
            total = total + jnp.where(wide >= taps - i, term, 0.0)
        return total, weights[taps - 1 : taps, :]

    q_past, q_tap = history(c.q_hist, v.q_hist, c.conv_query, v.conv_query)
    k_past, k_tap = history(c.k_hist, v.k_hist, c.conv_key, v.conv_key)
    v_past, v_tap = history(c.v_hist, v.v_hist, c.conv_value, v.conv_value)
    c.out_gain.wait()
    gain_out = v.out_gain[...].astype(F32)
    c.decay_log.wait()
    c.time_bias.wait()
    rate = jnp.exp(v.decay_log[...])
    bias = v.time_bias[...]
    mlp_row = gain_row(c.mlp_gain, v.mlp_gain)

    heard(4)
    phase("hubs")
    s_proj.leaves(False)
    s_proj.hubs()
    s_gate.leaves(True)
    s_gate.leaves(False)
    phase("gate_hubs")
    s_gate.hubs()
    for copy in (c.w_out, c.w_up, c.w_down, c.delta_state):
        copy.wait()

    phase("sums")
    sums = s_proj.total()
    phase("delta")
    at_v = 2 * key_cols
    misc = sums[:, at_v + value_cols :]
    scale = lax.rsqrt(misc[:, LANES - 1 : LANES] / width + EPSILON)
    misc = misc * scale

    def filtered(at, past, tap):
        value = sums[:, at : at + past.shape[1]] * scale * tap + past
        return value * jax.nn.sigmoid(value)

    def unit(values):
        return values * lax.rsqrt(jnp.sum(values * values, axis=-1, keepdims=True) + EPSILON)

    filtered_q = filtered(0, q_past, q_tap)
    filtered_k = filtered(key_cols, k_past, k_tap)
    values_now = filtered(at_v, v_past, v_tap)
    fade_all = jnp.exp(-rate * softplus(misc[:, :heads_all] + bias))
    strength_all = jax.nn.sigmoid(misc)

    def own_head(table, at):
        lanes = lax.broadcasted_iota(jnp.int32, table.shape, 1)
        one = jnp.sum(jnp.where(lanes == at, table, 0.0), axis=1, keepdims=True)
        return jnp.broadcast_to(one, (own, size))

    key_heads = key_cols // size
    repeat = heads // key_heads
    state = v.delta_state
    fades, strengths = [], []
    for h in range(heads):
        fades.append(jnp.where(lens == 1, 0.0, own_head(fade_all, tp * heads + h)))
        strengths.append(own_head(strength_all, heads_all + tp * heads + h))
    queries, keys, meets = [], [], []
    for g in range(key_heads):
        queries.append(unit(filtered_q[:, g * size : (g + 1) * size]) * size ** (-0.5))
        keys.append(unit(filtered_k[:, g * size : (g + 1) * size]))
        meet = jnp.sum(queries[g] * keys[g], axis=1, keepdims=True)
        meets.append(jnp.broadcast_to(meet, (own, size)))
    out_copies = []
    for s in range(own):
        for g in range(key_heads):
            key_wide = jnp.broadcast_to(keys[g][s : s + 1], (size, size)).T
            query_wide = jnp.broadcast_to(queries[g][s : s + 1], (size, size)).T
            for h in range(g * repeat, (g + 1) * repeat):
                held = state[s, h]
                fade = fades[h][s : s + 1]
                value = values_now[s : s + 1, h * size : (h + 1) * size]
                recalled = fade * jnp.sum(held * key_wide, axis=0, keepdims=True)
                update = strengths[h][s : s + 1] * (value - recalled)
                read = fade * jnp.sum(held * query_wide, axis=0, keepdims=True)
                r.readout[h, s : s + 1, :] = read + meets[g][s : s + 1] * update
                state[s, h] = fade * held + key_wide * update
        copy = pltpu.make_async_copy(state.at[s], new_state.at[s], r.out_sems.at[s])
        copy.start()
        out_copies.append(copy)

    phase("gated")
    gate_in = s_gate.total() * scale
    gated = []
    for h in range(heads):
        read = r.readout[h]
        mean = jnp.mean(read * read, axis=1, keepdims=True)
        gate = gate_in[:, h * size : (h + 1) * size]
        gate = gate * jax.nn.sigmoid(gate)
        gated.append(read * lax.rsqrt(mean + EPSILON) * gain_out * gate)
    r.all_gated[kv] = jnp.concatenate(gated, axis=1).astype(BF16)
    g_gated = Gather(over_kv(r.gated_sems), d.gated_tree, r.all_gated)
    g_gated.begin()
    phase("gather_gated")
    g_gated.finish()

    phase("mixer")

    def whole(blocks):
        return rows_of(blocks[...].astype(F32)).astype(BF16)

    mixer = jnp.dot(whole(r.all_gated), v.w_out[...], preferred_element_type=F32)
    r.mixers[0] = mixer.astype(BF16)
    x_mixer = over_tp(r.mixer_sems)
    others = sorted(ring_offsets(n_tp), key=lambda o: -abs(o))
    for o in others:
        x_mixer.start(o, o, r.mixers.at[0], r.mixers.at[o % n_tp])
    phase("sum_mixer")
    for o in reversed(others):
        x_mixer.wait(o, r.mixers.at[0], r.mixers.at[o % n_tp])
        mixer = mixer + r.mixers[o % n_tp].astype(F32)
    phase("up")
    mixed = (r.stream_block[...] + mixer).astype(BF16).astype(F32)
    r.mixed_turned[...] = mixed.T.reshape(n_tp, piece, seqs)

    lhs = by_owner((mixed * mlp_row).astype(BF16).astype(F32)).astype(BF16)
    put(r.part_u, 0, jnp.dot(lhs, v.w_up[...], preferred_element_type=F32))
    put(r.part_u, ff, spread_squares(mixed))
    s_up = Scatter(over_kv(r.up_sems), parents, r.part_u, r.send_u, r.recv_u)
    s_up.leaves(True)
    s_up.leaves(False)
    phase("up_hubs")
    s_up.hubs()
    phase("up_sums")
    sums = s_up.total()
    phase("hidden")
    unit_scale = lax.rsqrt(sums[:, ff : ff + 1] / width + EPSILON)
    raised = jnp.maximum(sums[:, :ff] * unit_scale, 0.0)
    r.all_hidden[kv] = (raised * raised).astype(BF16)
    g_hidden = Gather(over_kv(r.hidden_sems), d.hidden_tree, r.all_hidden)
    g_hidden.begin()
    phase("gather_hidden")
    g_hidden.finish()
    phase("down")
    down = lax.dot_general(
        v.w_down[...], whole(r.all_hidden), (((0,), (1,)), ((), ())), preferred_element_type=F32
    )
    down = down.reshape(n_tp, piece, seqs)
    r.down_wide[...] = down
    r.downs[...] = down.astype(BF16)
    x_down = over_tp(r.down_sems)
    for o in others:
        x_down.start(o, o, r.downs.at[x_down.at(o)], r.arrived.at[o % n_tp])
    phase("sum_down")
    total = r.down_wide[tp]
    for o in reversed(others):
        x_down.wait(o, r.downs.at[0], r.arrived.at[o % n_tp])
        total = total + r.arrived[o % n_tp].astype(F32)
    phase("leave")
    r.result[...] = (r.mixed_turned[tp] + total).astype(BF16)
    copy = pltpu.make_async_copy(r.result, result, r.out_sems.at[own])
    copy.start()
    out_copies.append(copy)
    exchanges = (x_stream, x_proj, s_gate.x, g_gated.x, x_mixer, s_up.x, g_hidden.x, x_down)
    for exchange in exchanges:
        exchange.drain()
    for copy in out_copies:
        copy.wait()
    phase.end()


def on_device(n_kv, n_tp, *args):
    given = Inputs(*args)
    own, heads, size = given.delta_state.shape[:3]
    key_cols, value_cols = given.q_hist.shape[2], given.v_hist.shape[2]
    taps = given.q_hist.shape[1] + 1
    width = given.norm_gain.shape[0]
    block = width // n_kv
    piece = block // n_tp
    ff = given.w_up.shape[1]
    heads_all = given.w_beta.shape[1]
    seqs = own * n_kv
    given = given._replace(
        stream=given.stream.T,
        q_hist=given.q_hist.transpose(1, 0, 2),
        k_hist=given.k_hist.transpose(1, 0, 2),
        v_hist=given.v_hist.transpose(1, 0, 2),
        norm_gain=given.norm_gain.reshape(n_kv, block),
        mlp_gain=given.mlp_gain.reshape(n_kv, block),
        w_beta=given.w_beta.T,
        w_decay=given.w_decay.T,
        decay_log=given.decay_log.reshape(1, -1),
        time_bias=given.time_bias.reshape(1, -1),
        out_gain=given.out_gain.reshape(1, -1),
    )
    d = types.SimpleNamespace(
        n_kv=n_kv,
        n_tp=n_tp,
        own=own,
        heads=heads,
        size=size,
        key_cols=key_cols,
        value_cols=value_cols,
        ff=ff,
        width=width,
        block=block,
        piece=piece,
        taps=taps,
        heads_all=heads_all,
        scatter_tree=tree(n_kv, (2, 4, 6, 8)),
        gated_tree=tree(n_kv, ()),
        hidden_tree=tree(n_kv, (2, 4, 6)),
    )
    held = Inputs(*[pltpu.VMEM(x.shape, x.dtype) for x in given])
    held = held._replace(
        lengths=pltpu.SMEM(given.lengths.shape, given.lengths.dtype),
        w_beta=pltpu.VMEM((heads_all, block), BF16),
        w_decay=pltpu.VMEM((heads_all, block), BF16),
        conv_query=pltpu.VMEM((taps, key_cols), BF16),
        conv_key=pltpu.VMEM((taps, key_cols), BF16),
        conv_value=pltpu.VMEM((taps, value_cols), BF16),
    )
    wide_a = 2 * key_cols + value_cols + LANES
    wide_u = ff + LANES

    def sems(n):
        return (pltpu.SemaphoreType.DMA((n,)), pltpu.SemaphoreType.DMA((n,)))

    def wide(*shape):
        return pltpu.VMEM(shape, F32)

    def narrow(*shape):
        return pltpu.VMEM(shape, BF16)

    scratch = dict(
        stream_sems=sems(n_tp),
        proj_sems=sems(n_kv),
        gate_sems=sems(n_kv),
        gated_sems=sems(n_kv),
        mixer_sems=sems(n_tp),
        up_sems=sems(n_kv),
        hidden_sems=sems(n_kv),
        down_sems=sems(n_tp),
        load_sems=pltpu.SemaphoreType.DMA((len(given),)),
        out_sems=pltpu.SemaphoreType.DMA((own + 1,)),
        near_sems=pltpu.SemaphoreType.REGULAR((3,)),
        pieces=narrow(n_tp, piece, seqs),
        rows=wide(n_kv, own, block),
        stream_block=wide(seqs, block),
        part_a=wide(n_kv, own, wide_a),
        send_a=narrow(n_kv, own, wide_a),
        recv_a=narrow(n_kv, own, wide_a),
        part_g=wide(n_kv, own, value_cols),
        send_g=narrow(n_kv, own, value_cols),
        recv_g=narrow(n_kv, own, value_cols),
        readout=wide(heads, own, size),
        all_gated=narrow(n_kv, own, value_cols),
        mixers=narrow(n_tp, seqs, block),
        mixed_turned=wide(n_tp, piece, seqs),
        part_u=wide(n_kv, own, wide_u),
        send_u=narrow(n_kv, own, wide_u),
        recv_u=narrow(n_kv, own, wide_u),
        all_hidden=narrow(n_kv, own, ff),
        downs=narrow(n_tp, piece, seqs),
        down_wide=wide(n_tp, piece, seqs),
        arrived=narrow(n_tp, piece, seqs),
        result=narrow(piece, seqs),
    )

    def kernel(*refs):
        count = len(given)
        a, outs, v = Inputs(*refs[:count]), refs[count : count + 2], refs[count + 2]
        layer(d, a, *outs, v, types.SimpleNamespace(**refs[count + 3]))

    state = given.delta_state
    turned, new_state = pl.pallas_call(
        kernel,
        out_shape=(
            jax.ShapeDtypeStruct((piece, seqs), BF16),
            jax.ShapeDtypeStruct(state.shape, state.dtype),
        ),
        in_specs=[pl.BlockSpec(memory_space=pl.ANY)] * len(given),
        out_specs=[pl.BlockSpec(memory_space=pl.ANY)] * 2,
        scratch_shapes=(held, scratch),
        compiler_params=pltpu.CompilerParams(
            collective_id=0, has_side_effects=True, vmem_limit_bytes=67043328
        ),
        name="layer",
    )(*given)
    return (turned.T, new_state)


def solution(mesh):
    kv_tp, heads_of = P("kv", "tp"), P("tp", "kv")
    history = P(("grp", "kv"), None, "tp")
    state = P(("grp", "kv"), "tp", None, None)
    stream = P("grp", ("kv", "tp"))
    placed = Inputs(*[P()] * len(Inputs._fields))._replace(
        stream=stream,
        lengths=P(("grp", "kv")),
        delta_state=state,
        q_hist=history,
        k_hist=history,
        v_hist=history,
        w_query=kv_tp,
        w_key=kv_tp,
        w_value=kv_tp,
        w_gate=kv_tp,
        w_out=heads_of,
        w_up=kv_tp,
        w_down=heads_of,
    )
    return jax.shard_map(
        functools.partial(on_device, mesh.shape["kv"], mesh.shape["tp"]),
        mesh=mesh,
        in_specs=tuple(placed),
        out_specs=(stream, state),
        check_vma=False,
    )
```

```python
import functools
import types
import typing

import jax
import jax.numpy as jnp
from jax import lax
from jax.experimental import pallas as pl
from jax.experimental.pallas import tpu as pltpu
from jax.sharding import PartitionSpec as P

EPSILON = 1e-06
LANES = 128
MESH = pl.DeviceIdType.MESH
F32 = jnp.float32
BF16 = jnp.bfloat16

PROJ = {7: 6, 8: 6, 4: 3, 5: 3}
GATED = {}
UP = {7: 6, 8: 6, 4: 3, 5: 3}
HIDDEN = {6: 5, 7: 5, 8: 5}
CHUNKS = 1

class Inputs(typing.NamedTuple):
    stream: typing.Any
    lengths: typing.Any
    delta_state: typing.Any
    q_hist: typing.Any
    k_hist: typing.Any
    v_hist: typing.Any
    norm_gain: typing.Any
    w_query: typing.Any
    w_key: typing.Any
    w_value: typing.Any
    w_gate: typing.Any
    w_beta: typing.Any
    w_decay: typing.Any
    conv_query: typing.Any
    conv_key: typing.Any
    conv_value: typing.Any
    decay_log: typing.Any
    time_bias: typing.Any
    out_gain: typing.Any
    w_out: typing.Any
    mlp_gain: typing.Any
    w_up: typing.Any
    w_down: typing.Any


def ring_offsets(n):
    return list(range(1, n // 2 + 1)) + [-o for o in range(1, (n + 1) // 2)]


def tree(n, relays):
    return {o: relays.get(abs(o), 0) * (1 if o > 0 else -1) for o in ring_offsets(n)}


def children_of(parents, o):
    return [c for c, p in parents.items() if p == o]


def depth_of(parents, o):
    return 0 if o == 0 else 1 + depth_of(parents, parents[o])


class Exchange:
    def __init__(self, axis, n, place, send_sems, recv_sems):
        self.axis, self.n, self.place = axis, n, place
        self.send_sems, self.recv_sems = send_sems, recv_sems
        self.started = []

    def at(self, o):
        return lax.rem(self.place + (o + self.n), self.n)

    def copy(self, key, hop, src, dst):
        slot = key % self.n
        return pltpu.make_async_remote_copy(
            src_ref=src,
            dst_ref=dst,
            send_sem=self.send_sems.at[slot],
            recv_sem=self.recv_sems.at[slot],
            device_id={self.axis: self.at(hop)},
            device_id_type=MESH,
        )

    def start(self, key, hop, src, dst):
        copy = self.copy(key, hop, src, dst)
        copy.start()
        self.started.append(copy)

    def wait(self, key, src, dst):
        self.copy(key, 1, src, dst).wait_recv()

    def drain(self):
        for copy in self.started:
            copy.wait_send()
        self.started = []


class Scatter:
    def __init__(self, exchange, parents, part, send, recv):
        self.x, self.parents = exchange, parents
        self.part, self.send, self.recv = part, send, recv
        self.inner = [o for o in parents if children_of(parents, o)]
        self.inner.sort(key=lambda o: (-depth_of(parents, o), -abs(o)))

    def _send(self, o, value):
        slot = o % self.x.n
        self.send[slot] = value.astype(BF16)
        self.x.start(o, o - self.parents[o], self.send.at[slot], self.recv.at[slot])

    def _gather(self, o):
        total = self.part[o % self.x.n]
        for c in children_of(self.parents, o):
            slot = c % self.x.n
            self.x.wait(c, self.send.at[slot], self.recv.at[slot])
            total = total + self.recv[slot].astype(F32)
        return total

    def leaves(self, among):
        for o in sorted(among, key=lambda o: (self.parents.get(o, 0) == 0, -abs(o))):
            if o != 0 and o not in self.inner:
                self._send(o, self.part[o % self.x.n])

    def hubs(self):
        for o in self.inner:
            self._send(o, self._gather(o))

    def total(self):
        return self._gather(0)


class Gather:
    def __init__(self, exchange, parents, blocks):
        self.x, self.parents, self.blocks = exchange, parents, blocks

    def _forward(self, o):
        source = self.blocks.at[self.x.at(-o)]
        for c in sorted(children_of(self.parents, o), key=lambda c: -abs(c)):
            self.x.start(c, c - o, source, source)

    def begin(self):
        self._forward(0)

    def finish(self, among=None):
        order = self.parents if among is None else [-o for o in among if o != 0]
        for o in sorted(order, key=lambda o: (not children_of(self.parents, o), abs(o))):
            block = self.blocks.at[self.x.at(-o)]
            self.x.wait(o, block, block)
            self._forward(o)


    @staticmethod
    def finish_all(gathers):
        parents = gathers[0].parents
        for o in sorted(parents, key=lambda o: (not children_of(parents, o), abs(o))):
            for gather in gathers:
                gather.finish([-o])


def rows_of(blocks):
    return blocks.reshape(blocks.shape[0] * blocks.shape[1], blocks.shape[2])


def softplus(x):
    return jnp.maximum(x, 0.0) + jnp.log1p(jnp.exp(-jnp.abs(x)))


class Phases:
    def __init__(self):
        self.scope = None

    def __call__(self, label):
        self.end()
        self.scope = jax.named_scope(label)
        self.scope.__enter__()

    def end(self):
        if self.scope is not None:
            self.scope.__exit__(None, None, None)
        self.scope = None


def layer(d, a, result, new_state, v, r):
    n_kv, n_tp = d.n_kv, d.n_tp
    own, heads, size = d.own, d.heads, d.size
    key_cols, value_cols, ff = d.key_cols, d.value_cols, d.ff
    width, block, piece, taps = d.width, d.block, d.piece, d.taps
    heads_all, seqs = d.heads_all, d.own * d.n_kv
    kv, tp = lax.axis_index("kv"), lax.axis_index("tp")
    phase = Phases()
    phase("enter")

    def over_kv(sems):
        return Exchange("kv", n_kv, kv, *sems)

    def over_tp(sems):
        return Exchange("tp", n_tp, tp, *sems)

    x_stream = over_tp(r.stream_sems)
    x_proj = over_kv(r.proj_sems[0])
    started = []

    def load(source, into):
        copy = pltpu.make_async_copy(source, into, r.load_sems.at[len(started)])
        copy.start()
        started.append(copy)
        return copy

    def tp_cols(ref, count):
        return ref.at[:, pl.ds(pl.multiple_of(tp * count, LANES), count)]

    def kv_cols(ref):
        return ref.at[:, pl.ds(pl.multiple_of(kv * block, LANES), block)]

    sources = a._replace(
        w_beta=kv_cols(a.w_beta),
        w_decay=kv_cols(a.w_decay),
        conv_query=tp_cols(a.conv_query, key_cols),
        conv_key=tp_cols(a.conv_key, key_cols),
        conv_value=tp_cols(a.conv_value, value_cols),
    )
    pieces = r.pieces
    stream_copy = load(a.stream, pieces.at[tp])
    barrier = pltpu.get_barrier_semaphore()
    for o in range(1, n_tp):
        pl.semaphore_signal(barrier, 1, device_id={"tp": x_stream.at(o)}, device_id_type=MESH)
    for o in (1, -1):
        pl.semaphore_signal(barrier, 1, device_id={"kv": x_proj.at(o)}, device_id_type=MESH)

    stream_copy.wait()
    pl.semaphore_wait(barrier, n_tp - 1 + 2)

    def tell(step):
        sem = r.near_sems.at[step.bit_length() - 1]
        for o in (step, -step):
            pl.semaphore_signal(sem, 1, device_id={"kv": x_proj.at(o)}, device_id_type=MESH)

    def heard(step):
        pl.semaphore_wait(r.near_sems.at[step.bit_length() - 1], 2)

    g_stream = Gather(x_stream, {o: 0 for o in ring_offsets(n_tp)}, pieces)
    g_stream.begin()
    tell(1)
    first = Inputs(*range(len(a)))
    order = [first.norm_gain, first.w_decay, first.w_beta]
    order += [first.w_query, first.w_key, first.w_value, first.w_gate]
    order += [i for i in range(len(a)) if i not in order]
    order.remove(first.stream)
    order.remove(first.delta_state)
    order.append(first.delta_state)
    copies = {i: load(sources[i], v[i]) for i in order}
    copies[first.stream] = stream_copy
    c = Inputs(*[copies[i] for i in range(len(a))])
    heard(1)
    tell(2)

    def gain_row(copy, ref):
        copy.wait()
        gains = ref[...].astype(F32)
        row = lax.broadcasted_iota(jnp.int32, gains.shape, 0)
        return jnp.sum(jnp.where(row == kv, gains, 0.0), axis=0, keepdims=True)

    norm_row = gain_row(c.norm_gain, v.norm_gain)
    c.w_decay.wait()
    c.w_beta.wait()
    idle = jnp.zeros((LANES - 2 * heads_all, block), F32)
    w_rates = [v.w_decay[...].astype(F32), v.w_beta[...].astype(F32), idle]
    w_rates = jnp.concatenate(w_rates, axis=0).astype(BF16)
    for copy in (c.w_query, c.w_key, c.w_value, c.w_gate):
        copy.wait()

    nearest = sorted([0] + ring_offsets(n_kv), key=lambda o: (abs(o), -o))
    near, far = nearest[: n_kv // 2], nearest[n_kv // 2 :]
    order = near + far

    def by_owner(values):
        r.rows[...] = values.reshape(n_kv, own, block)
        return jnp.concatenate([r.rows[x_proj.at(o)] for o in order], axis=0)

    def put(part, at, product, among):
        parts = product.reshape(len(among), own, product.shape[1])
        for i, o in enumerate(among):
            part[o % n_kv, :, at : at + product.shape[1]] = parts[i]

    def spread_squares(values):
        squares = jnp.sum(values * values, axis=1, keepdims=True)
        return by_owner(jnp.broadcast_to(squares, values.shape))

    phase("stream")
    g_stream.finish()
    heard(2)
    tell(4)
    phase("project")
    stream_block = rows_of(pieces[...].astype(F32)).T
    lhs = by_owner((stream_block * norm_row).astype(BF16).astype(F32)).astype(BF16)
    key_heads = key_cols // size
    repeat = heads // key_heads
    wide_v = repeat * size
    s_proj = []
    for g in range(key_heads):
        part, at = r.part_a[g], 0
        if g == 0:
            rates = lax.dot_general(
                lhs, w_rates, (((1,), (1,)), ((), ())), preferred_element_type=F32
            )
            lane = lax.broadcasted_iota(jnp.int32, rates.shape, 1)
            rates = jnp.where(lane < 2 * heads_all, rates, spread_squares(stream_block))
            put(part, 2 * size + 2 * wide_v, rates, order)
        for weight, count in ((v.w_query, size), (v.w_key, size), (v.w_value, wide_v), (v.w_gate, wide_v)):
            columns = weight[:, g * count : (g + 1) * count]
            put(part, at, jnp.dot(lhs, columns, preferred_element_type=F32), order)
            at += count
        s_proj.append(
            Scatter(over_kv(r.proj_sems[g]), d.proj_tree, part, r.send_a[g], r.recv_a[g])
        )
        s_proj[g].leaves([o for o in order if d.proj_tree.get(o, 0) != 0])
    r.stream_rows[...] = by_owner(stream_block)

    phase("history")
    c.lengths.wait()
    seq = lax.broadcasted_iota(jnp.int32, (own, LANES), 0)
    lens = jnp.zeros((own, LANES), jnp.int32)
    for s in range(own):
        lens = jnp.where(seq == s, v.lengths[s], lens)

    def history(past_copy, past, weight_copy, weight):
        past_copy.wait()
        weight_copy.wait()
        weights = weight[...].astype(F32)
        count = weights.shape[1]
        wide = jnp.concatenate([lens] * (count // LANES), axis=1)
        total = jnp.zeros((own, count), F32)
        for i in range(taps - 1):
            term = past[i].astype(F32) * weights[i : i + 1, :]
            total = total + jnp.where(wide >= taps - i, term, 0.0)
        return total, weights[taps - 1 : taps, :]

    q_past, q_tap = history(c.q_hist, v.q_hist, c.conv_query, v.conv_query)
    k_past, k_tap = history(c.k_hist, v.k_hist, c.conv_key, v.conv_key)
    v_past, v_tap = history(c.v_hist, v.v_hist, c.conv_value, v.conv_value)
    c.out_gain.wait()
    gain_out = v.out_gain[...].astype(F32)
    c.decay_log.wait()
    c.time_bias.wait()
    rate = jnp.exp(v.decay_log[...])
    bias = v.time_bias[...]
    mlp_row = gain_row(c.mlp_gain, v.mlp_gain)

    heard(4)
    phase("hubs")
    direct = [o for o in order if d.proj_tree.get(o, 0) == 0]
    for sums in s_proj:
        sums.leaves(direct)
    for sums in s_proj:
        sums.hubs()
    for copy in (c.w_out, c.w_up, c.w_down, c.delta_state):
        copy.wait()

    state = v.delta_state

    def unit(values):
        return values * lax.rsqrt(jnp.sum(values * values, axis=-1, keepdims=True) + EPSILON)

    def own_head(table, at):
        lanes = lax.broadcasted_iota(jnp.int32, table.shape, 1)
        one = jnp.sum(jnp.where(lanes == at, table, 0.0), axis=1, keepdims=True)
        return jnp.broadcast_to(one, (own, size))

    out_copies, g_gated = [], []
    for g in range(key_heads):
        phase("sums")
        sums = s_proj[g].total()
        phase("delta")
        if g == 0:
            misc = sums[:, 2 * size + 2 * wide_v :]
            scale = lax.rsqrt(misc[:, LANES - 1 : LANES] / width + EPSILON)
            misc = misc * scale
            fade_all = jnp.exp(-rate * softplus(misc[:, :heads_all] + bias))
            strength_all = jax.nn.sigmoid(misc)

        def filtered(at, past, tap, count):
            ours = slice(g * count, (g + 1) * count)
            value = sums[:, at : at + count] * scale * tap[:, ours] + past[:, ours]
            return value * jax.nn.sigmoid(value)

        query = unit(filtered(0, q_past, q_tap, size)) * size ** (-0.5)
        key = unit(filtered(size, k_past, k_tap, size))
        values_now = filtered(2 * size, v_past, v_tap, wide_v)
        gate_in = sums[:, 2 * size + wide_v : 2 * size + 2 * wide_v] * scale
        gate_in = gate_in * jax.nn.sigmoid(gate_in)
        meet = jnp.sum(query * key, axis=1, keepdims=True)
        ours = range(g * repeat, (g + 1) * repeat)
        fades = [jnp.where(lens == 1, 0.0, own_head(fade_all, tp * heads + h)) for h in ours]
        strengths = [own_head(strength_all, heads_all + tp * heads + h) for h in ours]
        for s in range(own):
            key_wide = jnp.broadcast_to(key[s : s + 1], (size, size)).T
            query_wide = jnp.broadcast_to(query[s : s + 1], (size, size)).T
            for i, h in enumerate(ours):
                held = state[s, h]
                fade = fades[i][s : s + 1]
                value = values_now[s : s + 1, i * size : (i + 1) * size]
                recalled = fade * jnp.sum(held * key_wide, axis=0, keepdims=True)
                update = strengths[i][s : s + 1] * (value - recalled)
                read = fade * jnp.sum(held * query_wide, axis=0, keepdims=True)
                r.readout[h, s : s + 1, :] = read + meet[s : s + 1] * update
                state[s, h] = fade * held + key_wide * update
        gated = []
        for i, h in enumerate(ours):
            read = r.readout[h]
            mean = jnp.mean(read * read, axis=1, keepdims=True)
            gate = gate_in[:, i * size : (i + 1) * size]
            gated.append(read * lax.rsqrt(mean + EPSILON) * gain_out * gate)
        r.all_gated[g][kv] = jnp.concatenate(gated, axis=1).astype(BF16)
        g_gated.append(Gather(over_kv(r.gated_sems[g]), d.gated_tree, r.all_gated[g]))
        g_gated[g].begin()
        heads_now = pl.ds(g * repeat, repeat)
        copy = pltpu.make_async_copy(
            state.at[:, heads_now], new_state.at[:, heads_now], r.out_sems.at[g]
        )
        copy.start()
        out_copies.append(copy)

    def rows_at(blocks, among):
        parts = [blocks[x_proj.at(o)].astype(F32) for o in among]
        return jnp.concatenate(parts, axis=0).astype(BF16)

    others = sorted(ring_offsets(n_tp), key=lambda o: -abs(o))
    halves = (near, far)
    x_mixer, mixers = [], []
    for i, among in enumerate(halves):
        phase("gather_gated")
        for gather in g_gated:
            gather.finish(among)
        phase("mixer")
        mixer = 0.0
        for g in range(key_heads):
            weights = v.w_out[g * wide_v : (g + 1) * wide_v, :]
            ours = rows_at(r.all_gated[g], among)
            mixer = mixer + jnp.dot(ours, weights, preferred_element_type=F32)
        mixers.append(mixer)
        r.mixers[i][0] = mixer.astype(BF16)
        x_mixer.append(over_tp(r.mixer_sems[i]))
        for o in others:
            x_mixer[i].start(o, o, r.mixers[i].at[0], r.mixers[i].at[o % n_tp])
    s_up = [
        Scatter(over_kv(r.up_sems[j]), d.up_tree, r.part_u[j], r.send_u[j], r.recv_u[j])
        for j in range(CHUNKS)
    ]
    wide_u = ff // CHUNKS
    at = 0
    for i, among in enumerate(halves):
        phase("sum_mixer")
        mixer = mixers[i]
        for o in reversed(others):
            x_mixer[i].wait(o, r.mixers[i].at[0], r.mixers[i].at[o % n_tp])
            mixer = mixer + r.mixers[i][o % n_tp].astype(F32)
        phase("up")
        count = own * len(among)
        mixed = (r.stream_rows[at : at + count, :] + mixer).astype(BF16).astype(F32)
        at += count
        blocks = mixed.reshape(len(among), own, block)
        for k, o in enumerate(among):
            r.rows[x_proj.at(o)] = blocks[k]
        lhs = (mixed * mlp_row).astype(BF16)
        for j in range(CHUNKS):
            weights = v.w_up[:, j * wide_u : (j + 1) * wide_u]
            put(r.part_u[j], 0, jnp.dot(lhs, weights, preferred_element_type=F32), among)
            s_up[j].leaves(among)
    turned = rows_of(r.rows[...]).T
    r.mixed_turned[...] = turned.reshape(n_tp, piece, seqs)
    r.squares[kv] = jnp.sum(turned * turned, axis=0, keepdims=True)
    g_squares = Gather(over_kv(r.square_sems), {o: 0 for o in ring_offsets(n_kv)}, r.squares)
    phase("up_hubs")
    for j in range(CHUNKS):
        s_up[j].hubs()
    g_squares.begin()
    g_hidden = []
    for j in range(CHUNKS):
        phase("up_sums")
        raised = jnp.maximum(s_up[j].total(), 0.0)
        phase("hidden")
        r.all_hidden[j][kv] = (raised * raised).astype(BF16)
        g_hidden.append(Gather(over_kv(r.hidden_sems[j]), d.hidden_tree, r.all_hidden[j]))
        g_hidden[j].begin()
    phase("gather_hidden")
    Gather.finish_all(g_hidden)
    phase("down")
    down = 0.0
    for j in range(CHUNKS):
        hidden = rows_of(r.all_hidden[j][...].astype(F32)).astype(BF16)
        weights = v.w_down[j * wide_u : (j + 1) * wide_u, :]
        down = down + lax.dot_general(
            weights, hidden, (((0,), (1,)), ((), ())), preferred_element_type=F32
        )
    down = down.reshape(n_tp, piece, seqs)
    r.down_wide[...] = down
    r.downs[...] = down.astype(BF16)
    x_down = over_tp(r.down_sems)
    for o in others:
        x_down.start(o, o, r.downs.at[x_down.at(o)], r.arrived.at[o % n_tp])
    phase("sum_down")
    g_squares.finish()
    squares = jnp.sum(r.squares[...], axis=0)
    unit_scale = lax.rsqrt(squares / width + EPSILON)
    total = r.down_wide[tp]
    for o in reversed(others):
        x_down.wait(o, r.downs.at[0], r.arrived.at[o % n_tp])
        total = total + r.arrived[o % n_tp].astype(F32)
    phase("leave")
    r.result[...] = (r.mixed_turned[tp] + total * (unit_scale * unit_scale)).astype(BF16)
    copy = pltpu.make_async_copy(r.result, result, r.out_sems.at[key_heads])
    copy.start()
    out_copies.append(copy)
    users = [*s_proj, *g_gated, *s_up, *g_hidden, g_squares]
    exchanges = [x_stream, x_down, *x_mixer] + [user.x for user in users]
    for exchange in exchanges:
        exchange.drain()
    for copy in out_copies:
        copy.wait()
    phase.end()


def on_device(n_kv, n_tp, *args):
    given = Inputs(*args)
    own, heads, size = given.delta_state.shape[:3]
    key_cols, value_cols = given.q_hist.shape[2], given.v_hist.shape[2]
    taps = given.q_hist.shape[1] + 1
    width = given.norm_gain.shape[0]
    block = width // n_kv
    piece = block // n_tp
    ff = given.w_up.shape[1]
    heads_all = given.w_beta.shape[1]
    seqs = own * n_kv
    given = given._replace(
        stream=given.stream.T,
        q_hist=given.q_hist.transpose(1, 0, 2),
        k_hist=given.k_hist.transpose(1, 0, 2),
        v_hist=given.v_hist.transpose(1, 0, 2),
        norm_gain=given.norm_gain.reshape(n_kv, block),
        mlp_gain=given.mlp_gain.reshape(n_kv, block),
        w_beta=given.w_beta.T,
        w_decay=given.w_decay.T,
        decay_log=given.decay_log.reshape(1, -1),
        time_bias=given.time_bias.reshape(1, -1),
        out_gain=given.out_gain.reshape(1, -1),
    )
    d = types.SimpleNamespace(
        n_kv=n_kv,
        n_tp=n_tp,
        own=own,
        heads=heads,
        size=size,
        key_cols=key_cols,
        value_cols=value_cols,
        ff=ff,
        width=width,
        block=block,
        piece=piece,
        taps=taps,
        heads_all=heads_all,
        proj_tree=tree(n_kv, PROJ),
        up_tree=tree(n_kv, UP),
        gated_tree=tree(n_kv, GATED),
        hidden_tree=tree(n_kv, HIDDEN),
    )
    held = Inputs(*[pltpu.VMEM(x.shape, x.dtype) for x in given])
    held = held._replace(
        lengths=pltpu.SMEM(given.lengths.shape, given.lengths.dtype),
        w_beta=pltpu.VMEM((heads_all, block), BF16),
        w_decay=pltpu.VMEM((heads_all, block), BF16),
        conv_query=pltpu.VMEM((taps, key_cols), BF16),
        conv_key=pltpu.VMEM((taps, key_cols), BF16),
        conv_value=pltpu.VMEM((taps, value_cols), BF16),
    )
    key_heads = key_cols // size
    wide_a = [2 * size + 2 * (value_cols // key_heads)] * key_heads
    wide_a[0] += LANES
    half = seqs // 2
    chunks = range(CHUNKS)

    def sems(n):
        return (pltpu.SemaphoreType.DMA((n,)), pltpu.SemaphoreType.DMA((n,)))

    def wide(*shape):
        return pltpu.VMEM(shape, F32)

    def narrow(*shape):
        return pltpu.VMEM(shape, BF16)

    scratch = dict(
        stream_sems=sems(n_tp),
        proj_sems=[sems(n_kv) for _ in wide_a],
        gated_sems=[sems(n_kv) for _ in wide_a],
        mixer_sems=[sems(n_tp) for _ in range(2)],
        up_sems=[sems(n_kv) for _ in chunks],
        hidden_sems=[sems(n_kv) for _ in chunks],
        down_sems=sems(n_tp),
        square_sems=sems(n_kv),
        load_sems=pltpu.SemaphoreType.DMA((len(given),)),
        out_sems=pltpu.SemaphoreType.DMA((key_heads + 1,)),
        near_sems=pltpu.SemaphoreType.REGULAR((3,)),
        pieces=narrow(n_tp, piece, seqs),
        rows=wide(n_kv, own, block),
        stream_rows=wide(seqs, block),
        part_a=[wide(n_kv, own, w) for w in wide_a],
        send_a=[narrow(n_kv, own, w) for w in wide_a],
        recv_a=[narrow(n_kv, own, w) for w in wide_a],
        readout=wide(heads, own, size),
        all_gated=[narrow(n_kv, own, value_cols // key_heads) for _ in wide_a],
        mixers=[narrow(n_tp, half, block) for _ in range(2)],
        mixed_turned=wide(n_tp, piece, seqs),
        part_u=[wide(n_kv, own, ff // CHUNKS) for _ in chunks],
        send_u=[narrow(n_kv, own, ff // CHUNKS) for _ in chunks],
        recv_u=[narrow(n_kv, own, ff // CHUNKS) for _ in chunks],
        squares=wide(n_kv, 1, seqs),
        all_hidden=[narrow(n_kv, own, ff // CHUNKS) for _ in chunks],
        downs=narrow(n_tp, piece, seqs),
        down_wide=wide(n_tp, piece, seqs),
        arrived=narrow(n_tp, piece, seqs),
        result=narrow(piece, seqs),
    )

    def kernel(*refs):
        count = len(given)
        a, outs, v = Inputs(*refs[:count]), refs[count : count + 2], refs[count + 2]
        layer(d, a, *outs, v, types.SimpleNamespace(**refs[count + 3]))

    state = given.delta_state
    turned, new_state = pl.pallas_call(
        kernel,
        out_shape=(
            jax.ShapeDtypeStruct((piece, seqs), BF16),
            jax.ShapeDtypeStruct(state.shape, state.dtype),
        ),
        in_specs=[pl.BlockSpec(memory_space=pl.ANY)] * len(given),
        out_specs=[pl.BlockSpec(memory_space=pl.ANY)] * 2,
        scratch_shapes=(held, scratch),
        compiler_params=pltpu.CompilerParams(
            collective_id=0, has_side_effects=True, vmem_limit_bytes=67043328
        ),
        name="layer",
    )(*given)
    return finish(turned, new_state)


def hand_on(turned, state, turned_out, state_out, turned_v, state_v, sems):
    chunks = state.shape[0]
    pairs = [(turned, turned_v, turned_out)]
    pairs += [(state.at[i], state_v.at[i], state_out.at[i]) for i in range(chunks)]
    reads = [pltpu.make_async_copy(p[0], p[1], sems.at[i]) for i, p in enumerate(pairs)]
    writes = [pltpu.make_async_copy(p[1], p[2], sems.at[i + len(pairs)]) for i, p in enumerate(pairs)]
    for copy in reads:
        copy.start()
    for read, write in zip(reads, writes):
        read.wait()
        write.start()
    for copy in writes:
        copy.wait()


def finish(turned, state):
    arrays = (turned, state)
    turned, state = pl.pallas_call(
        hand_on,
        out_shape=[jax.ShapeDtypeStruct(x.shape, x.dtype) for x in arrays],
        in_specs=[pl.BlockSpec(memory_space=pl.ANY)] * 2,
        out_specs=[pl.BlockSpec(memory_space=pl.ANY)] * 2,
        scratch_shapes=[pltpu.VMEM(x.shape, x.dtype) for x in arrays]
        + [pltpu.SemaphoreType.DMA((2 + 2 * state.shape[0],))],
        compiler_params=pltpu.CompilerParams(vmem_limit_bytes=67043328),
        name="hand_on",
    )(*arrays)
    return (turned.T, state)


def solution(mesh):
    kv_tp, heads_of = P("kv", "tp"), P("tp", "kv")
    history = P(("grp", "kv"), None, "tp")
    state = P(("grp", "kv"), "tp", None, None)
    stream = P("grp", ("kv", "tp"))
    placed = Inputs(*[P()] * len(Inputs._fields))._replace(
        stream=stream,
        lengths=P(("grp", "kv")),
        delta_state=state,
        q_hist=history,
        k_hist=history,
        v_hist=history,
        w_query=kv_tp,
        w_key=kv_tp,
        w_value=kv_tp,
        w_gate=kv_tp,
        w_out=heads_of,
        w_up=kv_tp,
        w_down=heads_of,
    )
    return jax.shard_map(
        functools.partial(on_device, mesh.shape["kv"], mesh.shape["tp"]),
        mesh=mesh,
        in_specs=tuple(placed),
        out_specs=(stream, state),
        check_vma=False,
    )
```
